32 devices in a mesh: sp: 4 (over z), tp: 4 (over y, x), dp: 2 (over core).
Axes of the slice: x: 2, y: 2, z: 4, core: 2. Of those that a mesh axis runs over, the one named last changes fastest.
Arguments:
- latent: bfloat16 [2, 4096, 2048], P('dp', 'sp'), may hold values from -4 to 4
- context: bfloat16 [2, 768, 2048], P('dp', 'sp'), may hold values from -6 to 6
- cond: float32 [2, 2048], P('dp'), may hold values from -6 to 6
- ctx_cond: float32 [2048], replicated, may hold values from -6 to 6
- norm_gain: float32 [2048], replicated, may hold values from 0.1 to 1.9
- mod_shift: bfloat16 [2048, 2048], P('sp', 'tp'), may hold values from -0.125 to 0.125
- mod_scale: bfloat16 [2048, 2048], P('sp', 'tp'), may hold values from -0.125 to 0.125
- mod_gate: bfloat16 [2048, 2048], P('sp', 'tp'), may hold values from -0.125 to 0.125
- w_query: bfloat16 [2048, 2048], P(None, 'tp'), may hold values from -0.125 to 0.125
- w_key: bfloat16 [2048, 512], P(None, 'tp'), may hold values from -0.125 to 0.125
- w_value: bfloat16 [2048, 512], P(None, 'tp'), may hold values from -0.125 to 0.125
- w_out: bfloat16 [2048, 2048], P('tp'), may hold values from -2 to 2
- q_gain: float32 [128], replicated, may hold values from 0.1 to 1.9
- k_gain: float32 [128], replicated, may hold values from 0.1 to 1.9
- sinks: float32 [16], P('tp'), may hold values from 3 to 8
Outputs:
- result: bfloat16 [2, 4096, 2048], P('dp', ('sp', 'tp'))
The draws below stay inside these ranges and needn't reach their ends.
All inputs are finite; a program needn't handle non-finite values.
Results may differ from the reference program's by a relative error of at most 0.013.
Values may be sent and summed in bfloat16 or wider, within the bound.
A program may use at most 128 MiB of HBM per device.

```python
import jax
import jax.numpy as jnp
from jax import lax

D = 2048
HEADS = 16
KV_HEADS = 4
HEAD_DIM = 128
WINDOW = 128
GRID_W = 64
CTX = 768
SEQ = 4096
BATCH = 2
N_TP = 4


def block_levels(own_key, shape, shards, least, high):
    level = 1.0
    for axis_at, shards_of in shards:
        heights = jax.random.uniform(jax.random.fold_in(jax.random.fold_in(own_key, 6), axis_at), (shards_of,), jnp.float32, least / len(shards), high / len(shards))
        level = level * jnp.repeat(jnp.exp(heights), shape[axis_at] // shards_of).reshape((-1,) + (1,) * (len(shape) - 1 - axis_at))
    return level


def gaussian(stream_key, extent, deviation, bound, split=(), held_as=jnp.bfloat16):
    values = jax.random.normal(stream_key, extent, jnp.float32) * deviation
    if len(split) > 0:
        values = block_levels(stream_key, extent, split, -0.22, 0.18) * values
    return jnp.clip(values, min=-bound, max=bound).astype(held_as)


def setup_inputs(seed: int = 0) -> dict:
    splits = jax.random.split(jax.random.key(seed), 16)
    latent = gaussian(splits[0], (BATCH, SEQ, D), 0.5, 4.0, ((0, 2), (1, 4)))
    context = gaussian(splits[1], (BATCH, CTX, D), 1.0, 6.0, ((0, 2), (1, 4)))
    cond = gaussian(splits[2], (BATCH, D), 1.0, 6.0, ((0, 2),), jnp.float32)
    ctx_cond = gaussian(splits[3], (D,), 1.0, 6.0, (), jnp.float32)
    norm_gain = jnp.clip(1.0 + 0.18 * jax.random.normal(splits[4], (D,), jnp.float32), 0.1, 1.9)
    mod_shift = gaussian(splits[5], (D, D), D ** -0.5, 0.125, ((0, 4), (1, 4)))
    mod_scale = gaussian(splits[6], (D, D), D ** -0.5, 0.125, ((0, 4), (1, 4)))
    mod_gate = gaussian(splits[7], (D, D), D ** -0.5, 0.125, ((0, 4), (1, 4)))
    w_query = gaussian(splits[8], (D, HEADS * HEAD_DIM), D ** -0.5, 0.125, ((1, 4),))
    w_key = gaussian(splits[9], (D, KV_HEADS * HEAD_DIM), D ** -0.5, 0.125, ((1, 4),))
    w_value = gaussian(splits[10], (D, KV_HEADS * HEAD_DIM), D ** -0.5, 0.125, ((1, 4),))
    w_out = gaussian(splits[11], (HEADS * HEAD_DIM, D), (max(HEADS * HEAD_DIM // 256, 1)) ** -0.5, 2.0, ((0, 4),))
    q_gain = jnp.clip(1.0 + 0.18 * jax.random.normal(splits[12], (HEAD_DIM,), jnp.float32), 0.1, 1.9)
    k_gain = jnp.clip(1.0 + 0.18 * jax.random.normal(splits[13], (HEAD_DIM,), jnp.float32), 0.1, 1.9)
    sinks = jnp.clip(3.0 + 5.0 * jax.random.uniform(splits[14], (HEADS,), jnp.float32) ** block_levels(splits[14], (HEADS,), ((0, 4),), -0.2, 0.2), 3.0, 8.0)
    return dict(latent=latent, context=context, cond=cond, ctx_cond=ctx_cond, norm_gain=norm_gain, mod_shift=mod_shift, mod_scale=mod_scale, mod_gate=mod_gate, w_query=w_query, w_key=w_key, w_value=w_value, w_out=w_out, q_gain=q_gain, k_gain=k_gain, sinks=sinks)


NORM_EPSILON = 1e-06
ROPE_BASE = 10000.0

def head_norm(vectors, gain_row):
    return vectors * lax.rsqrt(lax.optimization_barrier(jnp.mean(vectors * vectors, axis=-1, keepdims=True)) + NORM_EPSILON) * gain_row.astype(jnp.float32)

def modulated(rows_in, gain_row, shift_row, scale_row):
    values = rows_in.astype(jnp.float32)
    normed = values * lax.rsqrt(lax.optimization_barrier(jnp.mean(values * values, axis=-1, keepdims=True)) + NORM_EPSILON) * gain_row.astype(jnp.float32)
    return (normed * (1.0 + scale_row) + shift_row).astype(jnp.bfloat16)

def rotate_half(halves, coords):
    quarter = halves.shape[-1] // 2
    frequency = ROPE_BASE ** (-jnp.arange(quarter, dtype=jnp.float32) / quarter)
    angles = coords.astype(jnp.float32)[:, None] * frequency
    cosine_part = jnp.cos(angles)[:, None, :]
    sine_part = jnp.sin(angles)[:, None, :]
    first_part = halves[..., :quarter]
    second_part = halves[..., quarter:]
    return jnp.concatenate([first_part * cosine_part - second_part * sine_part, second_part * cosine_part + first_part * sine_part], axis=-1)

def rotate(vectors, positions):
    half_dim = vectors.shape[-1] // 2
    return jnp.concatenate([rotate_half(vectors[..., :half_dim], positions // GRID_W), rotate_half(vectors[..., half_dim:], positions % GRID_W)], axis=-1)

def window_attention(lat_queries, lat_keys, lat_values, ctx_keys, ctx_values, sinks):
    seq_len = lat_queries.shape[0]
    group_size = HEADS // KV_HEADS
    score_scale = HEAD_DIM ** (-0.5)
    block_count = seq_len // WINDOW
    query_blocks = lat_queries.reshape(block_count, WINDOW, KV_HEADS, group_size, HEAD_DIM)
    padded_keys = jnp.pad(lat_keys, ((WINDOW, WINDOW), (0, 0), (0, 0)))
    padded_values = jnp.pad(lat_values, ((WINDOW, WINDOW), (0, 0), (0, 0)))
    sink_exp = jnp.exp(sinks.astype(jnp.float32)).reshape(KV_HEADS, group_size)
    key_rows = jnp.arange(3 * WINDOW, dtype=jnp.int32)
    query_rows = jnp.arange(WINDOW, dtype=jnp.int32)
    offset_rows = key_rows[None, :] - query_rows[:, None]
    in_band = (offset_rows >= 0) & (offset_rows <= 2 * WINDOW)
    ctx_key_f = ctx_keys.astype(jnp.float32)
    ctx_value_f = ctx_values.astype(jnp.float32)

    def one_block(inputs):
        block_queries, block_index = inputs
        first_row = (block_index * WINDOW).astype(jnp.int32)
        block_keys = lax.dynamic_slice_in_dim(padded_keys, first_row, 3 * WINDOW, 0).astype(jnp.float32)
        block_values = lax.dynamic_slice_in_dim(padded_values, first_row, 3 * WINDOW, 0).astype(jnp.float32)
        key_pos = first_row - WINDOW + key_rows
        in_window = in_band & ((key_pos >= 0) & (key_pos < seq_len))[None, :]
        block_q = block_queries.astype(jnp.float32)
        scores = jnp.einsum('qhgd,khd->hgqk', block_q, block_keys) * score_scale
        weights = jnp.where(in_window, jnp.exp(scores), 0.0)
        ctx_weights = jnp.exp(jnp.einsum('qhgd,chd->hgqc', block_q, ctx_key_f) * score_scale)
        denominator = lax.optimization_barrier(jnp.sum(weights, axis=-1)) + lax.optimization_barrier(jnp.sum(ctx_weights, axis=-1)) + sink_exp[:, :, None]
        local_probs = (weights / denominator[..., None]).astype(jnp.bfloat16).astype(jnp.float32)
        ctx_probs = (ctx_weights / denominator[..., None]).astype(jnp.bfloat16).astype(jnp.float32)
        block_out = jnp.einsum('hgqk,khd->qhgd', local_probs, block_values) + jnp.einsum('hgqc,chd->qhgd', ctx_probs, ctx_value_f)
        return block_out.astype(jnp.bfloat16).reshape(WINDOW, HEADS * HEAD_DIM)
    attended = lax.map(one_block, (query_blocks, jnp.arange(block_count, dtype=jnp.int32)))
    return attended.reshape(seq_len, HEADS * HEAD_DIM)

def reference(latent, context, cond, ctx_cond, norm_gain, mod_shift, mod_scale, mod_gate, w_query, w_key, w_value, w_out, q_gain, k_gain, sinks):
    seq_len = latent.shape[1]
    ctx_len = context.shape[1]
    group_cols = HEADS * HEAD_DIM // N_TP
    outputs = []
    for sample in range(latent.shape[0]):
        active = jax.nn.silu(jnp.stack([cond[sample].astype(jnp.float32), ctx_cond.astype(jnp.float32)])).astype(jnp.bfloat16)
        shifts = jnp.dot(active, mod_shift, preferred_element_type=jnp.float32)
        scales = jnp.dot(active, mod_scale, preferred_element_type=jnp.float32)
        gate_rows = jnp.dot(active[0:1], mod_gate, preferred_element_type=jnp.float32)
        lat_in = modulated(latent[sample], norm_gain, shifts[0], scales[0])
        ctx_in = modulated(context[sample], norm_gain, shifts[1], scales[1])
        positions = jnp.arange(seq_len, dtype=jnp.int32)
        lat_queries = rotate(head_norm(jnp.dot(lat_in, w_query, preferred_element_type=jnp.float32).reshape(seq_len, HEADS, HEAD_DIM), q_gain), positions).astype(jnp.bfloat16)
        lat_keys = rotate(head_norm(jnp.dot(lat_in, w_key, preferred_element_type=jnp.float32).reshape(seq_len, KV_HEADS, HEAD_DIM), k_gain), positions).astype(jnp.bfloat16)
        lat_values = jnp.dot(lat_in, w_value, preferred_element_type=jnp.float32).astype(jnp.bfloat16).reshape(seq_len, KV_HEADS, HEAD_DIM)
        ctx_keys = head_norm(jnp.dot(ctx_in, w_key, preferred_element_type=jnp.float32).reshape(ctx_len, KV_HEADS, HEAD_DIM), k_gain).astype(jnp.bfloat16)
        ctx_values = jnp.dot(ctx_in, w_value, preferred_element_type=jnp.float32).astype(jnp.bfloat16).reshape(ctx_len, KV_HEADS, HEAD_DIM)
        attended = window_attention(lat_queries, lat_keys, lat_values, ctx_keys, ctx_values, sinks)
        mixed_rows = jnp.zeros((seq_len, D), jnp.float32)
        for group_index in range(N_TP):
            partial_value = jnp.dot(attended[:, group_index * group_cols:(group_index + 1) * group_cols], w_out[group_index * group_cols:(group_index + 1) * group_cols], preferred_element_type=jnp.float32).astype(jnp.bfloat16)
            mixed_rows = mixed_rows + lax.optimization_barrier(partial_value).astype(jnp.float32)
        result = latent[sample].astype(jnp.float32) + gate_rows[0] * mixed_rows
        outputs.append(result.astype(jnp.bfloat16))
    return jnp.stack(outputs)
```

```python
import functools
import math

import jax
import jax.numpy as jnp
from jax import lax
from jax.experimental import pallas as pl
from jax.experimental.pallas import tpu as pltpu
from jax.sharding import PartitionSpec as P

HEAD_DIM = 128
WINDOW = 128
GRID_W = 64
NORM_EPSILON = 1e-06
ROPE_BASE = 10000.0
SLICES = 2

F32 = jnp.float32
BF16 = jnp.bfloat16


def rows_rsqrt(x):
    mean = jnp.mean(x * x, axis=-1, keepdims=True)
    return lax.rsqrt(mean + NORM_EPSILON)


def dot(a, b):
    return jnp.dot(a, b, preferred_element_type=F32)


def dot_t(a, b):
    return lax.dot_general(a, b, (((1,), (1,)), ((), ())), preferred_element_type=F32)


def body(
    n_sp,
    n_tp,
    n_dp,
    active_ref,
    gain_ref,
    qg_ref,
    kg_ref,
    sink_ref,
    latent_hbm,
    context_hbm,
    shift_hbm,
    scale_hbm,
    gate_hbm,
    wq_hbm,
    wk_hbm,
    wv_hbm,
    wo_hbm,
    out_hbm,
    lat,
    ctx,
    mods,
    wqkv,
    wfull,
    mslot,
    mfull,
    rms,
    cosb,
    sinb,
    xin,
    qbuf,
    kvbuf,
    ctxbuf,
    bias,
    att,
    arecv,
    outv,
    lsem,
    osem,
    m1s,
    m1r,
    m2s,
    m2r,
    cs,
    cr,
    hs,
    hr,
    as_,
    ar,
    ws,
    wr,
):
    sp = lax.axis_index("sp")
    tp = lax.axis_index("tp")
    dp = lax.axis_index("dp")
    tokens, width = lat.shape
    ctx_rows = ctx.shape[0]
    slot_rows = ctxbuf.shape[0] // n_sp
    mod_cols = mods.shape[2]
    qw = wq_hbm.shape[1]
    kw = wk_hbm.shape[1]
    q_local = qw // HEAD_DIM
    sub_rows = tokens // n_tp
    per_dest = sub_rows // WINDOW
    chunk = xin.shape[0]
    n_chunks = tokens // chunk
    group_rows = wo_hbm.shape[0]
    half = group_rows // n_dp
    piece = half // SLICES

    def local(src, dst, i):
        return pltpu.make_async_copy(src, dst, lsem.at[i])

    loads = [
        local(shift_hbm, mods.at[0], 0),
        local(scale_hbm, mods.at[1], 1),
        local(gate_hbm, mods.at[2], 2),
        local(latent_hbm.at[0], lat, 3),
        local(context_hbm.at[0], ctx, 4),
        local(wk_hbm, wqkv.at[:, qw : qw + kw], 5),
        local(wv_hbm, wqkv.at[:, qw + kw : qw + 2 * kw], 6),
        local(wq_hbm, wqkv.at[:, 0:qw], 7),
        local(wo_hbm, wfull.at[tp], 8),
    ]
    for load in loads:
        load.start()

    kvbuf[0:WINDOW, :] = jnp.zeros((WINDOW, kvbuf.shape[1]), BF16)
    kvbuf[tokens + WINDOW : tokens + 2 * WINDOW, :] = jnp.zeros((WINDOW, kvbuf.shape[1]), BF16)
    kvbuf[:, 2 * HEAD_DIM :] = jnp.ones((kvbuf.shape[0], HEAD_DIM), BF16)
    ctxbuf[:, 2 * HEAD_DIM :] = jnp.ones((ctxbuf.shape[0], HEAD_DIM), BF16)
    mslot[0] = jnp.zeros(mslot.shape[1:], F32)

    barrier = pltpu.get_barrier_semaphore()
    for k in range(1, n_sp):
        pl.semaphore_signal(barrier, inc=1, device_id={"sp": lax.rem(sp + k, n_sp)}, device_id_type=pl.DeviceIdType.MESH)
    for k in range(1, n_tp):
        pl.semaphore_signal(barrier, inc=1, device_id={"tp": lax.rem(tp + k, n_tp)}, device_id_type=pl.DeviceIdType.MESH)
    for k in range(1, n_dp):
        pl.semaphore_signal(barrier, inc=1, device_id={"dp": lax.rem(dp + k, n_dp)}, device_id_type=pl.DeviceIdType.MESH)

    def remote(src, dst, s_sem, r_sem, axis, index):
        return pltpu.make_async_remote_copy(
            src_ref=src,
            dst_ref=dst,
            send_sem=s_sem,
            recv_sem=r_sem,
            device_id={axis: index},
            device_id_type=pl.DeviceIdType.MESH,
        )

    act = active_ref[...]
    for i in range(3):
        loads[i].wait()
        mslot[0, 2 * i : 2 * i + 2, :] = dot(act, mods[i])[0:2, :]
    pl.semaphore_wait(barrier, n_sp + n_tp + n_dp - 3)

    phase1 = [
        remote(mslot.at[0], mslot.at[k], m1s.at[k - 1], m1r.at[k - 1], "sp", lax.rem(sp + k, n_sp))
        for k in range(1, n_sp)
    ]
    for c in phase1:
        c.start()

    lane = lax.broadcasted_iota(jnp.int32, (GRID_W, HEAD_DIM), 1)
    sub = lax.broadcasted_iota(jnp.int32, (GRID_W, HEAD_DIM), 0)
    quarter = HEAD_DIM // 4
    freq = jnp.exp((lane % quarter).astype(F32) * (-math.log(ROPE_BASE) / quarter))
    sign = jnp.where(lane % (2 * quarter) < quarter, -1.0, 1.0)
    col_ang = sub.astype(F32) * freq
    col_cos, col_sin = jnp.cos(col_ang), jnp.sin(col_ang) * sign
    n_rows = tokens // GRID_W
    row_ang = (sp * n_rows + lax.broadcasted_iota(jnp.int32, (n_rows, HEAD_DIM), 0)).astype(F32) * freq[0:1]
    row_cos, row_sin = jnp.cos(row_ang), jnp.sin(row_ang) * sign[0:1]
    for g in range(n_rows):
        cosb[g * GRID_W : (g + 1) * GRID_W, :] = jnp.where(lane < 2 * quarter, row_cos[g : g + 1], col_cos)
        sinb[g * GRID_W : (g + 1) * GRID_W, :] = jnp.where(lane < 2 * quarter, row_sin[g : g + 1], col_sin)
    off = lax.broadcasted_iota(jnp.int32, (WINDOW, 3 * WINDOW), 1) - lax.broadcasted_iota(
        jnp.int32, (WINDOW, 3 * WINDOW), 0
    )
    bias[...] = jnp.where((off >= 0) & (off <= 2 * WINDOW), 0.0, -1e30)

    for c in phase1:
        c.wait()
    total = mslot[0]
    for k in range(1, n_sp):
        total = total + mslot[k]
    mfull[tp] = total
    phase2 = [
        remote(mfull.at[tp], mfull.at[tp], m2s.at[k - 1], m2r.at[k - 1], "tp", lax.rem(tp + k, n_tp))
        for k in range(1, n_tp)
    ]
    for c in phase2:
        c.start()

    near = tp + 1 - 2 * lax.rem(tp, 2)
    far = lax.rem(tp + 2, n_tp)
    diag = near + far - tp
    first = near + dp * (far - near)
    second = far + dp * (near - far)
    mate = lax.rem(dp + 1, n_dp)

    def wrows(core, j):
        return pl.ds(pl.multiple_of(core * half + j * piece, piece), piece)

    def wcopy(kind, j, src, slot, axis, index):
        i = kind * SLICES + j
        return remote(src, wfull.at[slot, wrows(dp, j), :], ws.at[i], wr.at[i], axis, index)

    own_first = [wcopy(0, j, wo_hbm.at[wrows(dp, j), :], tp, "tp", first) for j in range(SLICES)]
    own_second = [wcopy(1, j, wo_hbm.at[wrows(dp, j), :], tp, "tp", second) for j in range(SLICES)]

    def passed(kind, j, slot, axis, index):
        return wcopy(kind, j, wfull.at[slot, wrows(dp, j), :], slot, axis, index)

    relay = [passed(2, j, first, "tp", second) for j in range(SLICES)]
    share = [
        [passed(3 + i, j, slot, "dp", mate) for j in range(SLICES)]
        for i, slot in enumerate((first, second, diag))
    ]
    for j in range(SLICES):
        own_first[j].start()
        own_second[j].start()

    loads[3].wait()

    @pl.loop(0, tokens // 32)
    def _(i):
        rows = pl.ds(pl.multiple_of(i * 32, 32), 32)
        x = lat[rows, :].astype(F32)
        rms[rows, :] = jnp.broadcast_to(rows_rsqrt(x), (32, HEAD_DIM))

    for i in (4, 5, 6):
        loads[i].wait()
    x = ctx[...].astype(F32)
    ctx_r = rows_rsqrt(x)
    for c in phase2:
        c.wait()

    def mod_row(r):
        return jnp.concatenate([mfull[j, r : r + 1, :] for j in range(n_tp)], axis=1)

    gain = gain_ref[...]
    ctx_in = (x * ctx_r * (gain * (1.0 + mod_row(3))) + mod_row(1)).astype(BF16)
    ckv = dot(ctx_in, wqkv[:, qw : qw + 2 * kw])
    ck = ckv[:, :kw]
    kg = kg_ref[...]
    ck = ck * rows_rsqrt(ck) * kg
    if slot_rows != ctx_rows:
        ctxbuf[0:slot_rows, 0 : 2 * HEAD_DIM] = jnp.zeros((slot_rows, 2 * HEAD_DIM), BF16)
    ctxbuf[0:ctx_rows, 0:HEAD_DIM] = ck.astype(BF16)
    ctxbuf[0:ctx_rows, HEAD_DIM : 2 * HEAD_DIM] = ckv[:, kw:].astype(BF16)
    ctx_copies = [
        remote(
            ctxbuf.at[0:slot_rows, 0 : 2 * HEAD_DIM],
            ctxbuf.at[k * slot_rows : (k + 1) * slot_rows, 0 : 2 * HEAD_DIM],
            cs.at[k - 1],
            cr.at[k - 1],
            "sp",
            lax.rem(sp + k, n_sp),
        )
        for k in range(1, n_sp)
    ]
    for c in ctx_copies:
        c.start()

    loads[7].wait()
    amp = gain * (1.0 + mod_row(2))
    shift = mod_row(0)
    qg = qg_ref[...] * (HEAD_DIM**-0.5 * math.log2(math.e))
    lane_c = lax.broadcasted_iota(jnp.int32, (chunk, HEAD_DIM), 1)
    is_first = lane_c % (2 * quarter) < quarter

    up_row = tokens
    halo_up = remote(
        kvbuf.at[pl.ds(up_row, WINDOW), 0 : 2 * HEAD_DIM],
        kvbuf.at[pl.ds(0, WINDOW), 0 : 2 * HEAD_DIM],
        hs.at[0],
        hr.at[0],
        "sp",
        lax.rem(sp + 1, n_sp),
    )
    halo_down = remote(
        kvbuf.at[pl.ds(WINDOW, WINDOW), 0 : 2 * HEAD_DIM],
        kvbuf.at[pl.ds(tokens + WINDOW, WINDOW), 0 : 2 * HEAD_DIM],
        hs.at[1],
        hr.at[1],
        "sp",
        lax.rem(sp + n_sp - 1, n_sp),
    )

    @pl.loop(0, n_chunks)
    def _(c):
        base = pl.multiple_of(c * chunk, chunk)

        @pl.loop(0, chunk // 16)
        def _(i):
            src = pl.ds(pl.multiple_of(base + i * 16, 16), 16)
            r = rms[src, :]
            r = jnp.concatenate([r] * (width // HEAD_DIM), axis=1)
            y = lat[src, :].astype(F32) * r * amp + shift
            xin[pl.ds(pl.multiple_of(i * 16, 16), 16), :] = y.astype(BF16)

        y = dot(xin[...], wqkv[...])
        cos_t = cosb[pl.ds(base, chunk), :]
        sin_t = sinb[pl.ds(base, chunk), :]

        def turned(v, g):
            n = v * rows_rsqrt(v) * g
            swapped = jnp.where(
                is_first,
                pltpu.roll(n, HEAD_DIM - quarter, 1),
                pltpu.roll(n, quarter, 1),
            )
            return (n * cos_t + swapped * sin_t).astype(BF16)

        dst = pl.ds(pl.multiple_of(base + WINDOW, WINDOW), chunk)
        kvbuf[dst, 0:HEAD_DIM] = turned(y[:, qw : qw + kw], kg)
        kvbuf[dst, HEAD_DIM : 2 * HEAD_DIM] = y[:, qw + kw :].astype(BF16)
        blocks = chunk // WINDOW
        for h in range(q_local):
            q = turned(y[:, h * HEAD_DIM : (h + 1) * HEAD_DIM], qg)
            for b in range(blocks):
                qbuf[c * blocks + b, h * WINDOW : (h + 1) * WINDOW, :] = q[b * WINDOW : (b + 1) * WINDOW]

    @pl.when(sp < n_sp - 1)
    def _():
        halo_up.start()

    @pl.when(sp > 0)
    def _():
        halo_down.start()

    for c in ctx_copies:
        c.wait()

    @pl.when(sp < n_sp - 1)
    def _():
        halo_up.wait_send()
        halo_down.wait_recv()

    @pl.when(sp > 0)
    def _():
        halo_down.wait_send()
        halo_up.wait_recv()

    key_iota = lax.broadcasted_iota(jnp.int32, (1, 3 * WINDOW), 1)
    seq = tokens * n_sp
    if slot_rows != ctx_rows:
        pad_iota = lax.broadcasted_iota(jnp.int32, (1, ctxbuf.shape[0]), 1)
        pad_bias = jnp.where(pad_iota % slot_rows < ctx_rows, 0.0, -1e30)

    def send_att(j, dest):
        return remote(att.at[dest], arecv.at[tp], as_.at[j], ar.at[j], "tp", dest)

    @pl.loop(0, n_tp)
    def _(j):
        dest = lax.rem(tp + 1 + j, n_tp)

        @pl.loop(0, per_dest)
        def _(i):
            b = dest * per_dest + i
            q = qbuf[b]
            win = pl.ds(pl.multiple_of(b * WINDOW, WINDOW), 3 * WINDOW)
            key_pos = sp * tokens - WINDOW + b * WINDOW + key_iota
            edge = jnp.where((key_pos >= 0) & (key_pos < seq), 0.0, -1e30)
            s = dot_t(q, kvbuf[win, 0:HEAD_DIM])
            add = bias[...] + edge
            s = (s.reshape(q_local, WINDOW, 3 * WINDOW) + add[None]).reshape(q_local * WINDOW, 3 * WINDOW)
            p = jnp.exp2(s).astype(BF16)
            sc = dot_t(q, ctxbuf[:, 0:HEAD_DIM])
            if slot_rows != ctx_rows:
                sc = sc + pad_bias
            pc = jnp.exp2(sc).astype(BF16)
            o = dot(p, kvbuf[win, HEAD_DIM:]) + dot(pc, ctxbuf[:, HEAD_DIM:])
            for h in range(q_local):
                oh = o[h * WINDOW : (h + 1) * WINDOW]
                sink = jnp.exp(jnp.full((1, HEAD_DIM), sink_ref[h], F32))
                a = oh[:, :HEAD_DIM] / (oh[:, HEAD_DIM:] + sink)
                att[dest, pl.ds(pl.multiple_of(i * WINDOW, WINDOW), WINDOW), h * HEAD_DIM : (h + 1) * HEAD_DIM] = a.astype(BF16)

        @pl.when(j < n_tp - 1)
        def _():
            send_att(j, dest).start()

    for j in range(SLICES):
        own_first[j].wait()
        relay[j].start()
        share[0][j].start()
        own_second[j].wait()
        share[1][j].start()
    for j in range(SLICES):
        relay[j].wait()
        share[2][j].start()
    loads[8].wait()
    arecv[tp] = att[tp]
    for j in range(n_tp - 1):
        send_att(j, lax.rem(tp + 1 + j, n_tp)).wait()
    for kind in range(3):
        for j in range(SLICES):
            share[kind][j].wait()

    tile = 512 if width % 512 == 0 else width
    own = pl.ds(pl.multiple_of(tp * sub_rows, sub_rows), sub_rows)
    gate_tiles = mod_row(4)
    stores = []
    for n in range(width // tile):
        cols = slice(n * tile, (n + 1) * tile)
        acc = dot(arecv[0], wfull[0, :, cols])
        for g in range(1, n_tp):
            acc = acc + dot(arecv[g], wfull[g, :, cols])
        outv[:, cols] = (lat[own, cols].astype(F32) + gate_tiles[:, cols] * acc).astype(BF16)
        store = pltpu.make_async_copy(outv.at[:, cols], out_hbm.at[0, :, cols], osem.at[n])
        store.start()
        stores.append(store)
    for store in stores:
        store.wait()


def per_device(
    latent,
    context,
    cond,
    ctx_cond,
    norm_gain,
    mod_shift,
    mod_scale,
    mod_gate,
    w_query,
    w_key,
    w_value,
    w_out,
    q_gain,
    k_gain,
    sinks,
):
    n_sp, n_tp, n_dp = (lax.axis_size(a) for a in ("sp", "tp", "dp"))
    tokens, width = latent.shape[1:]
    ctx_rows = context.shape[1]
    part_rows, mod_cols = mod_shift.shape
    qw, kw = w_query.shape[1], w_key.shape[1]
    sub_rows = tokens // n_tp
    group_rows = w_out.shape[0]
    chunk = min(512, tokens)
    slot_rows = -(-ctx_rows // 16) * 16
    assert n_tp == 4 and n_dp == 2 and kw == HEAD_DIM
    cond_rows = jnp.stack([cond[0], ctx_cond])
    own_cond = lax.dynamic_slice_in_dim(cond_rows, lax.axis_index("sp") * part_rows, part_rows, 1)
    active = jnp.pad(jax.nn.silu(own_cond).astype(BF16), ((0, 14), (0, 0)))
    vmem = pl.BlockSpec(memory_space=pltpu.VMEM)
    hbm = pl.BlockSpec(memory_space=pl.ANY)
    dma = pltpu.SemaphoreType.DMA
    return pl.pallas_call(
        functools.partial(body, n_sp, n_tp, n_dp),
        out_shape=jax.ShapeDtypeStruct((1, sub_rows, width), BF16),
        in_specs=[vmem] * 4 + [pl.BlockSpec(memory_space=pltpu.SMEM)] + [hbm] * 9,
        out_specs=hbm,
        scratch_shapes=[
            pltpu.VMEM((tokens, width), BF16),
            pltpu.VMEM((ctx_rows, width), BF16),
            pltpu.VMEM((3, part_rows, mod_cols), BF16),
            pltpu.VMEM((width, qw + 2 * kw), BF16),
            pltpu.VMEM((n_tp, group_rows, width), BF16),
            pltpu.VMEM((n_sp, 8, mod_cols), F32),
            pltpu.VMEM((n_tp, 8, mod_cols), F32),
            pltpu.VMEM((tokens, HEAD_DIM), F32),
            pltpu.VMEM((tokens, HEAD_DIM), F32),
            pltpu.VMEM((tokens, HEAD_DIM), F32),
            pltpu.VMEM((chunk, width), BF16),
            pltpu.VMEM((tokens // WINDOW, qw // HEAD_DIM * WINDOW, HEAD_DIM), BF16),
            pltpu.VMEM((tokens + 2 * WINDOW, 3 * HEAD_DIM), BF16),
            pltpu.VMEM((n_sp * slot_rows, 3 * HEAD_DIM), BF16),
            pltpu.VMEM((WINDOW, 3 * WINDOW), F32),
            pltpu.VMEM((n_tp, sub_rows, qw), BF16),
            pltpu.VMEM((n_tp, sub_rows, qw), BF16),
            pltpu.VMEM((sub_rows, width), BF16),
            dma((9,)),
            dma((max(width // 512, 1),)),
            dma((n_sp - 1,)),
            dma((n_sp - 1,)),
            dma((n_tp - 1,)),
            dma((n_tp - 1,)),
            dma((n_sp - 1,)),
            dma((n_sp - 1,)),
            dma((2,)),
            dma((2,)),
            dma((n_tp - 1,)),
            dma((n_tp - 1,)),
            dma((6 * SLICES,)),
            dma((6 * SLICES,)),
        ],
        compiler_params=pltpu.CompilerParams(
            collective_id=0, has_side_effects=True, vmem_limit_bytes=60 * 1024 * 1024
        ),
    )(
        active,
        norm_gain[None],
        q_gain[None],
        k_gain[None],
        sinks,
        latent,
        context,
        mod_shift,
        mod_scale,
        mod_gate,
        w_query,
        w_key,
        w_value,
        w_out,
    )


def solution(mesh):
    in_specs = (
        P("dp", "sp", None),
        P("dp", "sp", None),
        P("dp", None),
        P(),
        P(),
        P("sp", "tp"),
        P("sp", "tp"),
        P("sp", "tp"),
        P(None, "tp"),
        P(None, "tp"),
        P(None, "tp"),
        P("tp", None),
        P(),
        P(),
        P("tp"),
    )
    out_specs = P("dp", ("sp", "tp"), None)
    return jax.shard_map(
        per_device, mesh=mesh, in_specs=in_specs, out_specs=out_specs, check_vma=False
    )
```

```python
import functools
import math

import jax
import jax.numpy as jnp
from jax import lax
from jax.experimental import pallas as pl
from jax.experimental.pallas import tpu as pltpu
from jax.sharding import PartitionSpec as P

HEAD_DIM = 128
WINDOW = 128
GRID_W = 64
NORM_EPSILON = 1e-06
ROPE_BASE = 10000.0
UNITS = 8
PASSED = 2

F32 = jnp.float32
BF16 = jnp.bfloat16


def rows_rsqrt(x):
    mean = jnp.mean(x * x, axis=-1, keepdims=True)
    return lax.rsqrt(mean + NORM_EPSILON)


def dot(a, b):
    return jnp.dot(a, b, preferred_element_type=F32)


def dot_t(a, b):
    return lax.dot_general(a, b, (((1,), (1,)), ((), ())), preferred_element_type=F32)


def body(
    n_sp,
    n_tp,
    n_dp,
    active_ref,
    gain_ref,
    qg_ref,
    kg_ref,
    sink_ref,
    latent_hbm,
    context_hbm,
    shift_hbm,
    scale_hbm,
    gate_hbm,
    wq_hbm,
    wk_hbm,
    wv_hbm,
    wo_hbm,
    out_hbm,
    lat,
    ctx,
    mods,
    wqkv,
    wfull,
    mslot,
    mfull,
    rms,
    cosb,
    sinb,
    xin,
    qbuf,
    kvbuf,
    ctxbuf,
    bias,
    att,
    arecv,
    outv,
    lsem,
    osem,
    m1s,
    m1r,
    m2s,
    m2r,
    cs,
    cr,
    hs,
    hr,
    as_,
    ar,
    ws,
    wr,
):
    sp = lax.axis_index("sp")
    tp = lax.axis_index("tp")
    dp = lax.axis_index("dp")
    tokens, width = lat.shape
    ctx_rows = ctx.shape[0]
    slot_rows = ctxbuf.shape[0] // n_sp
    mod_cols = mods.shape[2]
    qw = wq_hbm.shape[1]
    kw = wk_hbm.shape[1]
    q_local = qw // HEAD_DIM
    sub_rows = tokens // n_tp
    per_dest = sub_rows // WINDOW
    chunk = xin.shape[0]
    n_chunks = tokens // chunk
    group_rows = wo_hbm.shape[0]
    half = group_rows // n_dp
    unit = half // UNITS
    shared_units = UNITS - 2 * PASSED

    def local(src, dst, i):
        return pltpu.make_async_copy(src, dst, lsem.at[i])

    loads = [
        local(shift_hbm, mods.at[0], 0),
        local(scale_hbm, mods.at[1], 1),
        local(gate_hbm, mods.at[2], 2),
        local(latent_hbm.at[0], lat, 3),
        local(context_hbm.at[0], ctx, 4),
        local(wk_hbm, wqkv.at[:, qw : qw + kw], 5),
        local(wv_hbm, wqkv.at[:, qw + kw : qw + 2 * kw], 6),
        local(wq_hbm, wqkv.at[:, 0:qw], 7),
        local(wo_hbm, wfull.at[tp], 8),
    ]
    for load in loads[:3]:
        load.start()

    kvbuf[0:WINDOW, :] = jnp.zeros((WINDOW, kvbuf.shape[1]), BF16)
    kvbuf[tokens + WINDOW : tokens + 2 * WINDOW, :] = jnp.zeros((WINDOW, kvbuf.shape[1]), BF16)
    kvbuf[:, 2 * HEAD_DIM :] = jnp.ones((kvbuf.shape[0], HEAD_DIM), BF16)
    ctxbuf[:, 2 * HEAD_DIM :] = jnp.ones((ctxbuf.shape[0], HEAD_DIM), BF16)
    mslot[0] = jnp.zeros(mslot.shape[1:], F32)

    barrier = pltpu.get_barrier_semaphore()
    for k in range(1, n_sp):
        pl.semaphore_signal(barrier, inc=1, device_id={"sp": lax.rem(sp + k, n_sp)}, device_id_type=pl.DeviceIdType.MESH)
    for k in range(1, n_tp):
        pl.semaphore_signal(barrier, inc=1, device_id={"tp": lax.rem(tp + k, n_tp)}, device_id_type=pl.DeviceIdType.MESH)
    for k in range(1, n_dp):
        pl.semaphore_signal(barrier, inc=1, device_id={"dp": lax.rem(dp + k, n_dp)}, device_id_type=pl.DeviceIdType.MESH)

    def remote(src, dst, s_sem, r_sem, axis, index):
        return pltpu.make_async_remote_copy(
            src_ref=src,
            dst_ref=dst,
            send_sem=s_sem,
            recv_sem=r_sem,
            device_id={axis: index},
            device_id_type=pl.DeviceIdType.MESH,
        )

    near = tp + 1 - 2 * lax.rem(tp, 2)
    far = lax.rem(tp + 2, n_tp)
    diag = near + far - tp
    first = near + dp * (far - near)
    second = far + dp * (near - far)
    core_mate = lax.rem(dp + 1, n_dp)
    parity = lax.rem(sp, 2)
    sp_mate = sp + 1 - 2 * parity
    slots = (first, second, diag)
    n_direct = PASSED + 1

    def wrows(start, count):
        return pl.ds(pl.multiple_of(dp * half + start * unit, unit), count * unit)

    pieces = [wrows(parity * PASSED + j, 1) for j in range(PASSED)]
    pieces.append(wrows(2 * PASSED, shared_units))
    pieces += [wrows((1 - parity) * PASSED + j, 1) for j in range(PASSED)]

    def wcopy(i, src, slot, rows, axis, index):
        return remote(src, wfull.at[slot, rows, :], ws.at[i], wr.at[i], axis, index)

    def passed(i, slot, rows, axis, index):
        return wcopy(i, wfull.at[slot, rows, :], slot, rows, axis, index)

    to_first = [wcopy(j, wo_hbm.at[pieces[j], :], tp, pieces[j], "tp", first) for j in range(n_direct)]
    to_second = [
        wcopy(n_direct + j, wo_hbm.at[pieces[j], :], tp, pieces[j], "tp", second) for j in range(n_direct)
    ]
    relay = [passed(2 * n_direct + j, first, pieces[j], "tp", second) for j in range(n_direct)]
    at = 3 * n_direct
    over = [
        [passed(at + i * PASSED + j, slots[i], pieces[j], "sp", sp_mate) for j in range(PASSED)] for i in range(3)
    ]
    at += 3 * PASSED
    share = [
        [passed(at + i * len(pieces) + j, slots[i], pieces[j], "dp", core_mate) for j in range(len(pieces))]
        for i in range(3)
    ]

    def arrived(copies, i, j):
        copies[j].wait_recv()
        if j < PASSED:
            over[i][j].start()
        share[i][j].start()

    def direct_arrived(j):
        to_first[j].wait_recv()
        relay[j].start()
        share[0][j].start()
        to_second[j].wait_recv()
        share[1][j].start()

    act = active_ref[...]
    for i in range(3):
        loads[i].wait()
        mslot[0, 2 * i : 2 * i + 2, :] = dot(act, mods[i])[0:2, :]
    for load in loads[3:]:
        load.start()
    pl.semaphore_wait(barrier, n_sp + n_tp + n_dp - 3)

    phase1 = [
        remote(mslot.at[0], mslot.at[k], m1s.at[k - 1], m1r.at[k - 1], "sp", lax.rem(sp + k, n_sp))
        for k in range(1, n_sp)
    ]
    for c in phase1:
        c.start()
    to_first[0].start()
    to_second[0].start()

    lane = lax.broadcasted_iota(jnp.int32, (GRID_W, HEAD_DIM), 1)
    sub = lax.broadcasted_iota(jnp.int32, (GRID_W, HEAD_DIM), 0)
    quarter = HEAD_DIM // 4
    freq = jnp.exp((lane % quarter).astype(F32) * (-math.log(ROPE_BASE) / quarter))
    sign = jnp.where(lane % (2 * quarter) < quarter, -1.0, 1.0)
    col_ang = sub.astype(F32) * freq
    col_cos, col_sin = jnp.cos(col_ang), jnp.sin(col_ang) * sign
    n_rows = tokens // GRID_W
    row_ang = (sp * n_rows + lax.broadcasted_iota(jnp.int32, (n_rows, HEAD_DIM), 0)).astype(F32) * freq[0:1]
    row_cos, row_sin = jnp.cos(row_ang), jnp.sin(row_ang) * sign[0:1]
    for g in range(n_rows):
        cosb[g * GRID_W : (g + 1) * GRID_W, :] = jnp.where(lane < 2 * quarter, row_cos[g : g + 1], col_cos)
        sinb[g * GRID_W : (g + 1) * GRID_W, :] = jnp.where(lane < 2 * quarter, row_sin[g : g + 1], col_sin)
    off = lax.broadcasted_iota(jnp.int32, (WINDOW, 3 * WINDOW), 1) - lax.broadcasted_iota(
        jnp.int32, (WINDOW, 3 * WINDOW), 0
    )
    bias[...] = jnp.where((off >= 0) & (off <= 2 * WINDOW), 0.0, -1e30)

    for c in phase1:
        c.wait()
    total = mslot[0]
    for k in range(1, n_sp):
        total = total + mslot[k]
    mfull[tp] = total
    phase2 = [
        remote(mfull.at[tp], mfull.at[tp], m2s.at[k - 1], m2r.at[k - 1], "tp", lax.rem(tp + k, n_tp))
        for k in range(1, n_tp)
    ]
    for c in phase2:
        c.start()

    for j in range(1, n_direct):
        to_first[j].start()
        to_second[j].start()

    loads[3].wait()

    @pl.loop(0, tokens // 32)
    def _(i):
        rows = pl.ds(pl.multiple_of(i * 32, 32), 32)
        x = lat[rows, :].astype(F32)
        rms[rows, :] = jnp.broadcast_to(rows_rsqrt(x), (32, HEAD_DIM))

    for i in (4, 5, 6):
        loads[i].wait()
    x = ctx[...].astype(F32)
    ctx_r = rows_rsqrt(x)
    for c in phase2:
        c.wait()

    def mod_row(r):
        return jnp.concatenate([mfull[j, r : r + 1, :] for j in range(n_tp)], axis=1)

    gain = gain_ref[...]
    ctx_in = (x * ctx_r * (gain * (1.0 + mod_row(3))) + mod_row(1)).astype(BF16)
    ckv = dot(ctx_in, wqkv[:, qw : qw + 2 * kw])
    ck = ckv[:, :kw]
    kg = kg_ref[...]
    ck = ck * rows_rsqrt(ck) * kg
    if slot_rows != ctx_rows:
        ctxbuf[0:slot_rows, 0 : 2 * HEAD_DIM] = jnp.zeros((slot_rows, 2 * HEAD_DIM), BF16)
    ctxbuf[0:ctx_rows, 0:HEAD_DIM] = ck.astype(BF16)
    ctxbuf[0:ctx_rows, HEAD_DIM : 2 * HEAD_DIM] = ckv[:, kw:].astype(BF16)
    ctx_copies = [
        remote(
            ctxbuf.at[0:slot_rows, 0 : 2 * HEAD_DIM],
            ctxbuf.at[k * slot_rows : (k + 1) * slot_rows, 0 : 2 * HEAD_DIM],
            cs.at[k - 1],
            cr.at[k - 1],
            "sp",
            lax.rem(sp + k, n_sp),
        )
        for k in range(1, n_sp)
    ]
    for c in ctx_copies:
        c.start()
    direct_arrived(0)

    loads[7].wait()
    amp = gain * (1.0 + mod_row(2))
    shift = mod_row(0)
    qg = qg_ref[...] * (HEAD_DIM**-0.5 * math.log2(math.e))
    lane_c = lax.broadcasted_iota(jnp.int32, (chunk, HEAD_DIM), 1)
    is_first = lane_c % (2 * quarter) < quarter

    up_row = tokens
    halo_up = remote(
        kvbuf.at[pl.ds(up_row, WINDOW), 0 : 2 * HEAD_DIM],
        kvbuf.at[pl.ds(0, WINDOW), 0 : 2 * HEAD_DIM],
        hs.at[0],
        hr.at[0],
        "sp",
        lax.rem(sp + 1, n_sp),
    )
    halo_down = remote(
        kvbuf.at[pl.ds(WINDOW, WINDOW), 0 : 2 * HEAD_DIM],
        kvbuf.at[pl.ds(tokens + WINDOW, WINDOW), 0 : 2 * HEAD_DIM],
        hs.at[1],
        hr.at[1],
        "sp",
        lax.rem(sp + n_sp - 1, n_sp),
    )

    for c in range(n_chunks):
        base = c * chunk

        @pl.loop(0, chunk // 16)
        def _(i):
            src = pl.ds(pl.multiple_of(base + i * 16, 16), 16)
            r = rms[src, :]
            r = jnp.concatenate([r] * (width // HEAD_DIM), axis=1)
            y = lat[src, :].astype(F32) * r * amp + shift
            xin[pl.ds(pl.multiple_of(i * 16, 16), 16), :] = y.astype(BF16)

        y = dot(xin[...], wqkv[...])
        cos_t = cosb[pl.ds(base, chunk), :]
        sin_t = sinb[pl.ds(base, chunk), :]

        def turned(v, g):
            n = v * rows_rsqrt(v) * g
            swapped = jnp.where(
                is_first,
                pltpu.roll(n, HEAD_DIM - quarter, 1),
                pltpu.roll(n, quarter, 1),
            )
            return (n * cos_t + swapped * sin_t).astype(BF16)

        dst = pl.ds(base + WINDOW, chunk)
        kvbuf[dst, 0:HEAD_DIM] = turned(y[:, qw : qw + kw], kg)
        kvbuf[dst, HEAD_DIM : 2 * HEAD_DIM] = y[:, qw + kw :].astype(BF16)
        blocks = chunk // WINDOW
        for h in range(q_local):
            q = turned(y[:, h * HEAD_DIM : (h + 1) * HEAD_DIM], qg)
            for b in range(blocks):
                qbuf[c * blocks + b, h * WINDOW : (h + 1) * WINDOW, :] = q[b * WINDOW : (b + 1) * WINDOW]
        if c + 1 < PASSED:
            direct_arrived(c + 1)

    @pl.when(sp < n_sp - 1)
    def _():
        halo_up.start()

    @pl.when(sp > 0)
    def _():
        halo_down.start()

    for j in range(n_chunks + 1, PASSED):
        direct_arrived(j)
    for c in ctx_copies:
        c.wait()

    @pl.when(sp < n_sp - 1)
    def _():
        halo_up.wait_send()
        halo_down.wait_recv()

    @pl.when(sp > 0)
    def _():
        halo_down.wait_send()
        halo_up.wait_recv()

    for j in range(PASSED):
        over[0][j].start()
        over[1][j].start()

    key_iota = lax.broadcasted_iota(jnp.int32, (1, 3 * WINDOW), 1)
    seq = tokens * n_sp
    if slot_rows != ctx_rows:
        pad_iota = lax.broadcasted_iota(jnp.int32, (1, ctxbuf.shape[0]), 1)
        pad_bias = jnp.where(pad_iota % slot_rows < ctx_rows, 0.0, -1e30)

    def send_att(j, dest):
        return remote(att.at[dest], arecv.at[tp], as_.at[j], ar.at[j], "tp", dest)

    order = (diag, far, near, tp)
    for j, dest in enumerate(order):

        @pl.loop(0, per_dest)
        def _(i):
            b = dest * per_dest + i
            q = qbuf[b]
            win = pl.ds(pl.multiple_of(b * WINDOW, WINDOW), 3 * WINDOW)
            key_pos = sp * tokens - WINDOW + b * WINDOW + key_iota
            edge = jnp.where((key_pos >= 0) & (key_pos < seq), 0.0, -1e30)
            s = dot_t(q, kvbuf[win, 0:HEAD_DIM])
            add = bias[...] + edge
            s = (s.reshape(q_local, WINDOW, 3 * WINDOW) + add[None]).reshape(q_local * WINDOW, 3 * WINDOW)
            p = jnp.exp2(s).astype(BF16)
            sc = dot_t(q, ctxbuf[:, 0:HEAD_DIM])
            if slot_rows != ctx_rows:
                sc = sc + pad_bias
            pc = jnp.exp2(sc).astype(BF16)
            o = dot(p, kvbuf[win, HEAD_DIM:]) + dot(pc, ctxbuf[:, HEAD_DIM:])
            for h in range(q_local):
                oh = o[h * WINDOW : (h + 1) * WINDOW]
                sink = jnp.exp(jnp.full((1, HEAD_DIM), sink_ref[h], F32))
                a = oh[:, :HEAD_DIM] / (oh[:, HEAD_DIM:] + sink)
                att[dest, pl.ds(pl.multiple_of(i * WINDOW, WINDOW), WINDOW), h * HEAD_DIM : (h + 1) * HEAD_DIM] = a.astype(BF16)

        if j < n_tp - 1:
            send_att(j, dest).start()
        if j == 2:
            direct_arrived(PASSED)

    loads[8].wait()
    arecv[tp] = att[tp]
    for j in range(PASSED):
        arrived(relay, 2, j)
    for i in range(2):
        for j in range(PASSED):
            over[i][j].wait_recv()
            share[i][n_direct + j].start()
    arrived(relay, 2, PASSED)
    for j in range(PASSED):
        over[2][j].wait_recv()
        share[2][n_direct + j].start()
    for j in range(n_direct):
        to_first[j].wait_send()
        to_second[j].wait_send()
        relay[j].wait_send()
    for i in range(3):
        for j in range(PASSED):
            over[i][j].wait_send()
    for j in range(n_tp - 1):
        send_att(j, order[j]).wait()
    for i in range(3):
        for j in range(len(pieces)):
            share[i][j].wait()

    tile = 512 if width % 512 == 0 else width
    own = pl.ds(pl.multiple_of(tp * sub_rows, sub_rows), sub_rows)
    gate_tiles = mod_row(4)
    stores = []
    for n in range(width // tile):
        cols = slice(n * tile, (n + 1) * tile)
        acc = dot(arecv[0], wfull[0, :, cols])
        for g in range(1, n_tp):
            acc = acc + dot(arecv[g], wfull[g, :, cols])
        outv[:, cols] = (lat[own, cols].astype(F32) + gate_tiles[:, cols] * acc).astype(BF16)
        store = pltpu.make_async_copy(outv.at[:, cols], out_hbm.at[0, :, cols], osem.at[n])
        store.start()
        stores.append(store)
    for store in stores:
        store.wait()


def per_device(
    latent,
    context,
    cond,
    ctx_cond,
    norm_gain,
    mod_shift,
    mod_scale,
    mod_gate,
    w_query,
    w_key,
    w_value,
    w_out,
    q_gain,
    k_gain,
    sinks,
):
    n_sp, n_tp, n_dp = (lax.axis_size(a) for a in ("sp", "tp", "dp"))
    tokens, width = latent.shape[1:]
    ctx_rows = context.shape[1]
    part_rows, mod_cols = mod_shift.shape
    qw, kw = w_query.shape[1], w_key.shape[1]
    sub_rows = tokens // n_tp
    group_rows = w_out.shape[0]
    chunk = min(512, tokens)
    slot_rows = -(-ctx_rows // 16) * 16
    n_wsem = 3 * (PASSED + 1) + 3 * PASSED + 3 * (2 * PASSED + 1)
    assert n_sp % 2 == 0 and n_tp == 4 and n_dp == 2 and kw == HEAD_DIM
    cond_rows = jnp.stack([cond[0], ctx_cond])
    own_cond = lax.dynamic_slice_in_dim(cond_rows, lax.axis_index("sp") * part_rows, part_rows, 1)
    active = jnp.pad(jax.nn.silu(own_cond).astype(BF16), ((0, 14), (0, 0)))
    vmem = pl.BlockSpec(memory_space=pltpu.VMEM)
    hbm = pl.BlockSpec(memory_space=pl.ANY)
    dma = pltpu.SemaphoreType.DMA
    return pl.pallas_call(
        functools.partial(body, n_sp, n_tp, n_dp),
        out_shape=jax.ShapeDtypeStruct((1, sub_rows, width), BF16),
        in_specs=[vmem] * 4 + [pl.BlockSpec(memory_space=pltpu.SMEM)] + [hbm] * 9,
        out_specs=hbm,
        scratch_shapes=[
            pltpu.VMEM((tokens, width), BF16),
            pltpu.VMEM((ctx_rows, width), BF16),
            pltpu.VMEM((3, part_rows, mod_cols), BF16),
            pltpu.VMEM((width, qw + 2 * kw), BF16),
            pltpu.VMEM((n_tp, group_rows, width), BF16),
            pltpu.VMEM((n_sp, 8, mod_cols), F32),
            pltpu.VMEM((n_tp, 8, mod_cols), F32),
            pltpu.VMEM((tokens, HEAD_DIM), F32),
            pltpu.VMEM((tokens, HEAD_DIM), F32),
            pltpu.VMEM((tokens, HEAD_DIM), F32),
            pltpu.VMEM((chunk, width), BF16),
            pltpu.VMEM((tokens // WINDOW, qw // HEAD_DIM * WINDOW, HEAD_DIM), BF16),
            pltpu.VMEM((tokens + 2 * WINDOW, 3 * HEAD_DIM), BF16),
            pltpu.VMEM((n_sp * slot_rows, 3 * HEAD_DIM), BF16),
            pltpu.VMEM((WINDOW, 3 * WINDOW), F32),
            pltpu.VMEM((n_tp, sub_rows, qw), BF16),
            pltpu.VMEM((n_tp, sub_rows, qw), BF16),
            pltpu.VMEM((sub_rows, width), BF16),
            dma((9,)),
            dma((max(width // 512, 1),)),
            dma((n_sp - 1,)),
            dma((n_sp - 1,)),
            dma((n_tp - 1,)),
            dma((n_tp - 1,)),
            dma((n_sp - 1,)),
            dma((n_sp - 1,)),
            dma((2,)),
            dma((2,)),
            dma((n_tp - 1,)),
            dma((n_tp - 1,)),
            dma((n_wsem,)),
            dma((n_wsem,)),
        ],
        compiler_params=pltpu.CompilerParams(
            collective_id=0, has_side_effects=True, vmem_limit_bytes=60 * 1024 * 1024
        ),
    )(
        active,
        norm_gain[None],
        q_gain[None],
        k_gain[None],
        sinks,
        latent,
        context,
        mod_shift,
        mod_scale,
        mod_gate,
        w_query,
        w_key,
        w_value,
        w_out,
    )


def solution(mesh):
    in_specs = (
        P("dp", "sp", None),
        P("dp", "sp", None),
        P("dp", None),
        P(),
        P(),
        P("sp", "tp"),
        P("sp", "tp"),
        P("sp", "tp"),
        P(None, "tp"),
        P(None, "tp"),
        P(None, "tp"),
        P("tp", None),
        P(),
        P(),
        P("tp"),
    )
    out_specs = P("dp", ("sp", "tp"), None)
    return jax.shard_map(
        per_device, mesh=mesh, in_specs=in_specs, out_specs=out_specs, check_vma=False
    )
```
